32 devices in a mesh: sp: 8 (over z, y), tp: 4 (over x, core).
Axes of the slice: x: 2, y: 2, z: 4, core: 2. Of those that a mesh axis runs over, the one named last changes fastest.
Arguments:
- tokens: bfloat16 [4096, 2048], P(('sp', 'tp')), may hold values from -6 to 6
- norm_gain: float32 [2048], replicated, may hold values from 0.25 to 5
- w_query_one: bfloat16 [2048, 512], P(None, 'tp'), may hold values from -0.21875 to 0.21875
- w_query_two: bfloat16 [2048, 512], P(None, 'tp'), may hold values from -0.21875 to 0.21875
- w_key_one: bfloat16 [2048, 512], P(None, 'tp'), may hold values from -0.125 to 0.125
- w_key_two: bfloat16 [2048, 512], P(None, 'tp'), may hold values from -0.125 to 0.125
- w_value: bfloat16 [2048, 1024], P(None, 'tp'), may hold values from -0.125 to 0.125
- mix_lambda: float32 [8], P('tp'), may hold values from 0.3 to 0.8
- head_gain: float32 [128], replicated, may hold values from 0.1 to 1.9
- w_ret_query: bfloat16 [2048, 512], P(None, 'tp'), may hold values from -0.125 to 0.125
- w_ret_key: bfloat16 [2048, 512], P(None, 'tp'), may hold values from -0.125 to 0.125
- w_ret_value: bfloat16 [2048, 1024], P(None, 'tp'), may hold values from -0.125 to 0.125
- retain_log: float32 [8, 4096], P('tp', 'sp'), may hold values from -1 to 0
- init_state: float32 [8, 64, 128], P('tp'), may hold values from -144 to 144
- w_out_diff: bfloat16 [1024, 2048], P('tp'), may hold values from -0.125 to 0.125
- w_out_ret: bfloat16 [1024, 2048], P('tp'), may hold values from -0.125 to 0.125
Outputs:
- mixed: bfloat16 [4096, 2048], P(('sp', 'tp'))
The draws below stay inside these ranges and needn't reach their ends.
All inputs are finite; a program needn't handle non-finite values.
Results may differ from the reference program's by a relative error of at most 0.015.
The reference program's roundings to bfloat16 on the way count: a program that leaves them out, or rounds other values in their place, can miss the bound.
Values may be sent and summed in bfloat16 or wider, within the bound.
A program may use at most 128 MiB of HBM per device.

```python
import math
import jax
import jax.numpy as jnp
from jax import lax

D = 2048
HEADS_DIFF = 8
HEADS_RET = 8
HEAD = 64
VAL = 128
BLOCK = 256
TOK_DEV = 512
TOKENS = 4096


def draw_retain_log(key, part):
    keys = jax.random.split(jax.random.fold_in(key, 11), 7)
    slow = jax.random.bernoulli(keys[0], 0.5, (HEADS_RET,))
    slow_rate = jax.random.uniform(keys[1], (HEADS_RET,), minval=0.1, maxval=0.3) / TOKENS
    fast_rate = jnp.exp(jax.random.uniform(keys[2], (HEADS_RET,), minval=math.log(1.0 / 100.0), maxval=math.log(1.0 / 30.0)))
    fading_speed = jnp.where(slow, slow_rate, fast_rate)
    pace = jnp.exp(jax.random.uniform(keys[3], (TOKENS // TOK_DEV,), minval=-0.7, maxval=0.7))
    fading_speeds_list = jnp.repeat(pace, TOK_DEV)
    sampled_displacement = jnp.exp(jax.random.uniform(keys[4], (HEADS_RET, TOKENS), minval=-0.5, maxval=0.5))
    sequence_indices = jax.random.randint(keys[5], (HEADS_RET, 3), 0, TOKENS)
    stack_level = jnp.log(jax.random.uniform(keys[6], (HEADS_RET, 3), minval=0.5, maxval=0.8))
    sequence_index = jnp.arange(TOKENS, dtype=jnp.int32)
    cluster_sets = jnp.sum(jnp.where(sequence_index[None, None, :] == sequence_indices[:, :, None], stack_level[:, :, None], 0.0), axis=1)
    return (-fading_speed[:, None] * fading_speeds_list[None, :] * sampled_displacement + cluster_sets).astype(jnp.float32)


def draw_norm_gain(key, part):
    inner = jax.random.fold_in(key, 23)
    gains = 1.0 + 0.18 * jax.random.truncated_normal(inner, -4.0, 4.0, (D,))
    return gains.astype(jnp.float32)


def block_levels(stream_key, extent, pieces, low, largest):
    loudness, own = 1.0, jax.random.fold_in(stream_key, 6)
    for axis_at, parts in pieces:
        steps = jnp.exp(jax.random.uniform(jax.random.fold_in(own, axis_at), (parts,), jnp.float32, low / len(pieces), largest / len(pieces)))
        loudness = loudness * jnp.repeat(steps, extent[axis_at] // parts).reshape([-1 if axis == axis_at else 1 for axis in range(len(extent))])
    return loudness


def normal_values(own_key, dims, width, most, cuts=(), kind=jnp.bfloat16):
    gain = block_levels(own_key, dims, cuts, -0.22, 0.18) if cuts else 1.0
    entries = jax.random.normal(own_key, dims, jnp.float32) * width * gain
    return jnp.minimum(jnp.maximum(entries, -most), most).astype(kind)


def setup_inputs(seed: int = 0) -> dict:
    seeds = jax.random.split(jax.random.key(seed), 17)
    return {
        "tokens": normal_values(seeds[0], (TOKENS, D), 1.0, 6.0, ((0, 32),)),
        "norm_gain": draw_norm_gain(jax.random.fold_in(seeds[16], 71), 0),
        "w_query_one": normal_values(seeds[2], (D, HEADS_DIFF * HEAD), (D // 3) ** -0.5, 0.21875, ((1, 4),)),
        "w_query_two": normal_values(seeds[3], (D, HEADS_DIFF * HEAD), (D // 3) ** -0.5, 0.21875, ((1, 4),)),
        "w_key_one": normal_values(seeds[4], (D, HEADS_DIFF * HEAD), D ** -0.5, 0.125, ((1, 4),)),
        "w_key_two": normal_values(seeds[5], (D, HEADS_DIFF * HEAD), D ** -0.5, 0.125, ((1, 4),)),
        "w_value": normal_values(seeds[6], (D, HEADS_DIFF * VAL), D ** -0.5, 0.125, ((1, 4),)),
        "mix_lambda": jnp.clip(0.3 + 0.5 * jax.random.uniform(seeds[7], (HEADS_DIFF,), jnp.float32) ** block_levels(seeds[7], (HEADS_DIFF,), ((0, 4),), -0.2, 0.2), 0.3, 0.8),
        "head_gain": jnp.clip(1.0 + 0.18 * jax.random.normal(seeds[8], (VAL,), jnp.float32), 0.1, 1.9),
        "w_ret_query": normal_values(seeds[9], (D, HEADS_RET * HEAD), D ** -0.5, 0.125, ((1, 4),)),
        "w_ret_key": normal_values(seeds[10], (D, HEADS_RET * HEAD), D ** -0.5, 0.125, ((1, 4),)),
        "w_ret_value": normal_values(seeds[11], (D, HEADS_RET * VAL), D ** -0.5, 0.125, ((1, 4),)),
        "retain_log": draw_retain_log(jax.random.fold_in(seeds[16], 71), 0),
        "init_state": normal_values(seeds[13], (HEADS_RET, HEAD, VAL), 24.0, 144.0, ((0, 4),), jnp.float32),
        "w_out_diff": normal_values(seeds[14], (HEADS_DIFF * VAL, D), ((HEADS_DIFF + HEADS_RET) * VAL) ** -0.5, 0.125, ((0, 4),)),
        "w_out_ret": normal_values(seeds[15], (HEADS_RET * VAL, D), ((HEADS_DIFF + HEADS_RET) * VAL) ** -0.5, 0.125, ((0, 4),)),
    }


NORM_EPS = 1e-06
HEAD_EPS = 1e-05
DIFF_SCALE = 0.8
HIGHEST = lax.Precision.HIGHEST

def head_norm(values):
    return values * lax.rsqrt(lax.optimization_barrier(jnp.mean(values * values, axis=-1, keepdims=True)) + HEAD_EPS)

def diff_head(query_one, query_two, key_one, key_two, values, weight_two):
    total_rows = query_one.shape[0]
    block_rows = math.gcd(total_rows, 512)
    key_pos = jnp.arange(total_rows, dtype=jnp.int32)

    def one_block(number):
        begin_at = (number * block_rows).astype(jnp.int32)
        allowed = (begin_at + jnp.arange(block_rows, dtype=jnp.int32))[:, None] >= key_pos[None, :]

        def soft_map(query, keys):
            portion = lax.dynamic_slice_in_dim(query, begin_at, block_rows, 0)
            scores = jnp.dot(portion, keys.T, preferred_element_type=jnp.float32) * HEAD ** (-0.5)
            scores = jnp.where(allowed, scores, -jnp.inf)
            shifted = jnp.exp(scores - lax.optimization_barrier(jnp.max(scores, axis=-1, keepdims=True)))
            weighted = jnp.dot(shifted.astype(jnp.bfloat16), values, preferred_element_type=jnp.float32)
            return weighted / lax.optimization_barrier(jnp.sum(shifted, axis=-1, keepdims=True))
        return soft_map(query_one, key_one) - weight_two * soft_map(query_two, key_two)
    blocks = lax.map(one_block, jnp.arange(total_rows // block_rows, dtype=jnp.int32))
    return blocks.reshape(total_rows, VAL)

def retention(ret_query, ret_key, ret_value, retain_log, init_state):
    nblocks = TOKENS // BLOCK

    def split_blocks(data, size):
        return data.reshape(nblocks, BLOCK, HEADS_RET, size).transpose(0, 2, 1, 3)
    block_query = split_blocks(ret_query, HEAD)
    block_key = split_blocks(ret_key, HEAD)
    block_value = split_blocks(ret_value, VAL)
    log_blocks = retain_log.reshape(HEADS_RET, nblocks, BLOCK).transpose(1, 0, 2)
    sequence_index = jnp.arange(BLOCK, dtype=jnp.int32)
    causal = sequence_index[:, None] >= sequence_index[None, :]

    def ret_step(memory, inputs):
        query, keys, values, logs = inputs
        query_f = query.astype(jnp.float32)
        keys_f = keys.astype(jnp.float32)
        values_f = values.astype(jnp.float32)
        cumulative = jnp.cumsum(logs, axis=-1)
        gap_log = jnp.where(causal[None], cumulative[:, :, None] - cumulative[:, None, :], -jnp.inf)
        raw = jnp.einsum('hqd,hkd->hqk', query_f, keys_f, precision=HIGHEST)
        decayed = (raw * HEAD ** (-0.5) * jnp.exp(gap_log)).astype(jnp.bfloat16).astype(jnp.float32)
        result = jnp.einsum('hqk,hke->hqe', decayed, values_f, precision=HIGHEST)
        result = result + jnp.einsum('hqd,hde->hqe', query_f * jnp.exp(cumulative)[:, :, None], memory, precision=HIGHEST)
        last_log = cumulative[:, -1:]
        key_scaled = (keys_f * HEAD ** (-0.5) * jnp.exp(last_log - cumulative)[:, :, None]).astype(jnp.bfloat16).astype(jnp.float32)
        memory = jnp.exp(last_log)[:, :, None] * memory + jnp.einsum('hkd,hke->hde', key_scaled, values_f, precision=HIGHEST)
        return (memory, result)
    final_state, outputs = lax.scan(ret_step, init_state, (block_query, block_key, block_value, log_blocks))
    outputs = outputs.transpose(0, 2, 1, 3).reshape(TOKENS, HEADS_RET, VAL)
    return head_norm(outputs).reshape(TOKENS, HEADS_RET * VAL).astype(jnp.bfloat16)

def reference(tokens, norm_gain, w_query_one, w_query_two, w_key_one, w_key_two, w_value, mix_lambda, head_gain, w_ret_query, w_ret_key, w_ret_value, retain_log, init_state, w_out_diff, w_out_ret):
    floats = tokens.astype(jnp.float32)
    normed = (floats * lax.rsqrt(lax.optimization_barrier(jnp.mean(floats * floats, axis=-1, keepdims=True)) + NORM_EPS) * norm_gain).astype(jnp.bfloat16)

    def project(weight):
        return jnp.dot(normed, weight, preferred_element_type=jnp.float32).astype(jnp.bfloat16)
    query_one = project(w_query_one).reshape(TOKENS, HEADS_DIFF, HEAD)
    query_two = project(w_query_two).reshape(TOKENS, HEADS_DIFF, HEAD)
    key_one = project(w_key_one).reshape(TOKENS, HEADS_DIFF, HEAD)
    key_two = project(w_key_two).reshape(TOKENS, HEADS_DIFF, HEAD)
    values = project(w_value).reshape(TOKENS, HEADS_DIFF, VAL)
    head_outs = []
    for number in range(HEADS_DIFF):
        head_outs.append(diff_head(query_one[:, number], query_two[:, number], key_one[:, number], key_two[:, number], values[:, number], mix_lambda[number]))
    mixed_heads = jnp.stack(head_outs, axis=1)
    diff_out = (head_norm(mixed_heads) * head_gain * DIFF_SCALE).reshape(TOKENS, HEADS_DIFF * VAL).astype(jnp.bfloat16)
    ret_out = retention(project(w_ret_query), project(w_ret_key), project(w_ret_value), retain_log, init_state)
    total = jnp.dot(diff_out, w_out_diff, preferred_element_type=jnp.float32) + jnp.dot(ret_out, w_out_ret, preferred_element_type=jnp.float32)
    return total.astype(jnp.bfloat16)
```

```python
import functools

import jax
import jax.numpy as jnp
from jax import lax
from jax.experimental import pallas as pl
from jax.experimental.pallas import tpu as pltpu
from jax.sharding import PartitionSpec as P

BLOCK = 256
NORM_EPS = 1e-06
HEAD_EPS = 1e-05
DIFF_SCALE = 0.8
HIGHEST = lax.Precision.HIGHEST
MESH = pl.DeviceIdType.MESH
F32 = jnp.float32
BF16 = jnp.bfloat16
VMEM_LIMIT = 60 * 1024 * 1024


def remote(src, dst, send, recv, where):
    return pltpu.make_async_remote_copy(
        src_ref=src, dst_ref=dst, send_sem=send, recv_sem=recv,
        device_id=where, device_id_type=MESH,
    )


def head_norm(values):
    return values * lax.rsqrt(jnp.mean(values * values, axis=-1, keepdims=True) + HEAD_EPS)


def nn(a, b, **kw):
    return lax.dot_general(a, b, (((1,), (0,)), ((), ())), preferred_element_type=F32, **kw)


def nt(a, b):
    return lax.dot_general(a, b, (((1,), (1,)), ((), ())), preferred_element_type=F32)


def tn(a, b):
    return lax.dot_general(a, b, (((0,), (0,)), ((), ())), preferred_element_type=F32)


def project_kernel(ntp, widths, tokens_ref, gain_ref, *refs):
    nw = len(widths)
    w_refs = refs[:nw]
    q_ref, kv_ref, r_ref = refs[nw : nw + 3]
    gat, wbuf, wsem, pair_send, cross_send, recv = refs[nw + 3 :]
    me = lax.axis_index("tp")
    core = lax.rem(me, 2)
    chip = me // 2
    nchip = ntp // 2
    pair = me + 1 - 2 * core
    rows = tokens_ref.shape[0]
    barrier = pltpu.get_barrier_semaphore()
    pl.semaphore_signal(barrier, inc=1, device_id={"tp": pair}, device_id_type=MESH)
    for d in range(1, nchip):
        there = lax.rem(chip + d, nchip) * 2 + core
        pl.semaphore_signal(barrier, inc=1, device_id={"tp": there}, device_id_type=MESH)
    loads = []
    at = 0
    for n, width in enumerate(widths):
        loads.append(pltpu.make_async_copy(w_refs[n], wbuf.at[:, at : at + width], wsem.at[n]))
        loads[-1].start()
        at += width
    floats = tokens_ref[...].astype(F32)
    gat[me] = (
        floats * lax.rsqrt(jnp.mean(floats * floats, axis=-1, keepdims=True) + NORM_EPS) * gain_ref[...]
    ).astype(BF16)
    pl.semaphore_wait(barrier, nchip)
    crosses = []
    for d in range(1, nchip):
        there = lax.rem(chip + d, nchip) * 2 + core
        for half in range(2):
            part = pl.ds(half * (rows // 2), rows // 2)
            copy = remote(gat.at[me, part], gat.at[me, part], cross_send.at[d, half],
                          recv.at[me, half], {"tp": there})
            copy.start()
            crosses.append(copy)
    pairs = []

    def to_pair(which, half):
        part = pl.ds(half * (rows // 2), rows // 2)
        copy = remote(gat.at[which, part], gat.at[which, part], pair_send.at[which // 2, half],
                      recv.at[which, half], {"tp": pair})
        copy.start()
        pairs.append(copy)

    def landed(which, half):
        part = pl.ds(half * (rows // 2), rows // 2)
        remote(gat.at[which, part], gat.at[which, part], pair_send.at[which // 2, half],
               recv.at[which, half], {"tp": pair}).wait_recv()

    outs = (q_ref, kv_ref, r_ref)
    total = sum(widths)
    kinds = [(0, 2), (2, 5), (5, 8)]

    def project(which_chip):
        both = gat[pl.ds(which_chip * 2, 2)].reshape(2 * rows, gat.shape[2])
        where = pl.ds(pl.multiple_of(which_chip * 2 * rows, 2 * rows), 2 * rows)
        for out, (lo, hi) in zip(outs, kinds):
            start = sum(widths[:lo])
            span = sum(widths[lo:hi])
            cut = 256 if span % 256 == 0 else span
            for c in range(0, span, cut):
                out[where, c : c + cut] = nn(both, wbuf[:, start + c : start + c + cut]).astype(BF16)

    for half in range(2):
        to_pair(me, half)
    for load in loads:
        load.wait()
    for half in range(2):
        landed(pair, half)
    project(chip)
    for d in range(1, nchip):
        other = lax.rem(chip + nchip - d, nchip)
        for half in range(2):
            landed(other * 2 + core, half)
            to_pair(other * 2 + core, half)
        for half in range(2):
            landed(other * 2 + 1 - core, half)
        project(other)
    for copy in crosses + pairs:
        copy.wait_send()


def mix_kernel(nsp, heads, rheads, lam_ref, gain_ref, log_ref, init_ref, q_ref, r_ref, kv_hbm,
               out_ref, kvs, sts, qs, peak, den, acc, rmid, upd, ownsem, sem_z, sem_y, sem_rk,
               sem_zs, sem_ys, sem_rs):
    me = lax.axis_index("sp")
    b = lax.rem(me, 2)
    p = me // 2
    npair = nsp // 2
    rows, qw = q_ref.shape
    kw = qw // 2
    hd = kw // heads
    val = gain_ref.shape[1]
    up = {"sp": lax.rem(me + 2, nsp)}
    side = {"sp": me + 1 - 2 * b}
    own = pltpu.make_async_copy(kv_hbm, kvs.at[me], ownsem)
    own.start()
    barrier = pltpu.get_barrier_semaphore()
    pl.semaphore_signal(barrier, inc=1, device_id=side, device_id_type=MESH)

    @pl.when(p > 0)
    def _():
        pl.semaphore_signal(barrier, inc=1, device_id={"sp": lax.rem(me + nsp - 2, nsp)}, device_id_type=MESH)

    @pl.when(p < npair - 1)
    def _():
        pl.semaphore_signal(barrier, inc=1, device_id=up, device_id_type=MESH)

    pl.semaphore_wait(barrier, 1 + jnp.minimum(p, 1) + jnp.minimum(npair - 1 - p, 1))

    def kv_copy(i, j, sem, where):
        return remote(kvs.at[j], kvs.at[j], sem.at[i], sem_rk.at[j], where)

    def st_copy(i, j, sem, where):
        return remote(sts.at[j], sts.at[j], sem.at[i], sem_rs.at[j], where)

    own.wait()
    first_up = p < npair - 1

    @pl.when(first_up)
    def _():
        kv_copy(0, me, sem_z, up).start()

    @pl.when(b == 0)
    def _():
        kv_copy(0, me, sem_y, side).start()

    blk = BLOCK
    nblk = rows // blk
    vw = rheads * val
    rkw = rheads * hd
    tt = lax.broadcasted_iota(jnp.int32, (blk, blk), 0)
    uu = lax.broadcasted_iota(jnp.int32, (blk, blk), 1)
    lane = lax.broadcasted_iota(jnp.int32, (blk, rkw), 1)
    srow = lax.broadcasted_iota(jnp.int32, (rkw, val), 0)
    decays = []
    span_state = jnp.zeros((rkw, val), F32)
    span_logs = []
    for h in range(rheads):
        mine = (lane >= h * hd) & (lane < (h + 1) * hd)
        keep = (srow >= h * hd) & (srow < (h + 1) * hd)
        state = jnp.zeros((rkw, val), F32)
        log_all = jnp.zeros((1, 1), F32)
        for n in range(nblk):
            at = slice(n * blk, (n + 1) * blk)
            row = log_ref[h : h + 1, at]
            full = jnp.broadcast_to(row, (blk, blk))
            c_col = jnp.sum(jnp.where(uu <= tt, full, 0.0), axis=1, keepdims=True)
            l_col = jnp.sum(jnp.where(uu == tt, full, 0.0), axis=1, keepdims=True)
            c_row = jnp.sum(jnp.where(tt <= uu, l_col, 0.0), axis=0, keepdims=True)
            last = c_col[blk - 1 : blk, :]
            query = jnp.where(mine, r_ref[at, :rkw].astype(F32), 0.0)
            keys = r_ref[at, rkw : 2 * rkw]
            values = r_ref[at, 2 * rkw + h * val : 2 * rkw + (h + 1) * val]
            raw = nt(query.astype(BF16), keys)
            gap = jnp.where(uu <= tt, c_col - c_row, -jnp.inf)
            g = (raw * hd ** (-0.5) * jnp.exp(gap)).astype(BF16)
            rmid[h, at, :] = nn(g, values)
            kd = (keys.astype(F32) * hd ** (-0.5) * jnp.exp(last - c_col)).astype(BF16)
            new = jnp.where(keep, tn(kd, values), 0.0)
            upd[h, n] = new
            state = jnp.exp(last) * state + new
            log_all = log_all + last
            decays.append((c_col, last))
        span_state = span_state + state
        span_logs.append(log_all)
    sts[me, :rkw, :] = span_state.astype(BF16)
    for h in range(rheads):
        wide = jnp.broadcast_to(span_logs[h], (16, val))
        hi = wide.astype(BF16)
        sts[me, rkw + 32 * h : rkw + 32 * h + 16, :] = hi
        sts[me, rkw + 32 * h + 16 : rkw + 32 * h + 32, :] = (wide - hi.astype(F32)).astype(BF16)

    qlane = lax.broadcasted_iota(jnp.int32, (rows, kw), 1)
    for m in range(2):
        piece = q_ref[:, m * kw : (m + 1) * kw].astype(F32) * hd ** (-0.5)
        for h in range(heads):
            mine = (qlane >= h * hd) & (qlane < (h + 1) * hd)
            qs[m * heads + h] = jnp.where(mine, piece, 0.0).astype(BF16)
    qb = min(rows, 256)

    def attend(j, diagonal):
        @pl.loop(0, 2 * heads)
        def _(mh):
            m = mh // heads
            h = lax.rem(mh, heads)
            kcol = pl.ds(pl.multiple_of(m * kw, kw), kw)
            vcol = pl.ds(pl.multiple_of(2 * kw + h * val, val), val)
            for n in range(rows // qb):
                at = slice(n * qb, (n + 1) * qb)
                count = (n + 1) * qb if diagonal else rows
                scores = nt(qs[mh, at, :], kvs[j, :count, kcol])
                if diagonal:
                    ti = lax.broadcasted_iota(jnp.int32, (qb, count), 0) + n * qb
                    ui = lax.broadcasted_iota(jnp.int32, (qb, count), 1)
                    scores = jnp.where(ui <= ti, scores, -jnp.inf)
                top = jnp.max(scores, axis=1, keepdims=True)
                if not diagonal:
                    old = peak[mh, at, :]
                    top = jnp.maximum(old, top)
                e = jnp.exp(scores - top[:, :1])
                part = e[:, :128]
                for c in range(128, count, 128):
                    part = part + e[:, c : c + 128]
                weighted = nn(e.astype(BF16), kvs[j, :count, vcol])
                if diagonal:
                    peak[mh, at, :] = jnp.broadcast_to(top, (qb, 128))
                    den[mh, at, :] = part
                    acc[mh, at, :] = weighted
                else:
                    rescale = jnp.exp(old - top)
                    peak[mh, at, :] = top
                    den[mh, at, :] = den[mh, at, :] * rescale + part
                    acc[mh, at, :] = acc[mh, at, :] * rescale[:, :1] + weighted

    attend(me, True)

    @pl.when(first_up)
    def _():
        st_copy(0, me, sem_zs, up).start()

    @pl.when(b == 0)
    def _():
        st_copy(0, me, sem_ys, side).start()

    @pl.loop(1, npair + 1)
    def _(i):
        jz = 2 * (p - i) + b
        jy = 2 * (p - i + 1) + 1 - b

        @pl.when(i <= p)
        def _():
            kv_copy(i, jz, sem_z, up).wait_recv()

            @pl.when(first_up)
            def _():
                kv_copy(i, jz, sem_z, up).start()

            kv_copy(i, jz, sem_y, side).start()
            st_copy(i, jz, sem_zs, up).wait_recv()

            @pl.when(first_up)
            def _():
                st_copy(i, jz, sem_zs, up).start()

            st_copy(i, jz, sem_ys, side).start()
            attend(jz, False)

        @pl.when((i - 1 <= p) & ((b == 1) | (i > 1)))
        def _():
            kv_copy(i, jy, sem_y, side).wait_recv()
            st_copy(i, jy, sem_ys, side).wait_recv()
            attend(jy, False)

    for h in range(heads):
        pieces = []
        for m in range(2):
            mh = m * heads + h
            total = jnp.sum(den[mh], axis=1, keepdims=True)
            pieces.append(acc[mh] / total)
        mixed = pieces[0] - lam_ref[h] * pieces[1]
        out_ref[:, h * val : (h + 1) * val] = (head_norm(mixed) * gain_ref[...] * DIFF_SCALE).astype(BF16)

    first = []
    for h in range(rheads):
        parts = [jnp.zeros((hd, val), F32)] * h + [init_ref[h]] + [jnp.zeros((hd, val), F32)] * (rheads - 1 - h)
        first.append(jnp.concatenate(parts, axis=0) if rheads > 1 else parts[0])

    def join(j, states):
        out = []
        for h in range(rheads):
            keep = (srow >= h * hd) & (srow < (h + 1) * hd)
            base = rkw + 32 * h
            log = sts[j, base : base + 16, :].astype(F32) + sts[j, base + 16 : base + 32, :].astype(F32)
            piece = jnp.where(keep, sts[j, :rkw, :].astype(F32), 0.0)
            out.append(jnp.exp(log[:1, :]) * states[h] + piece)
        return tuple(out)

    carried = lax.fori_loop(0, me, join, tuple(first))
    for h in range(rheads):
        state = carried[h]
        for n in range(nblk):
            at = slice(n * blk, (n + 1) * blk)
            c_col, last = decays[h * nblk + n]
            query = r_ref[at, :rkw].astype(F32) * jnp.exp(c_col)
            result = rmid[h, at, :] + nn(query, state, precision=HIGHEST)
            if n + 1 < nblk:
                state = jnp.exp(last) * state + upd[h, n]
            out_ref[at, heads * val + h * val : heads * val + (h + 1) * val] = head_norm(result).astype(BF16)

    @pl.loop(0, npair)
    def _(i):
        j = 2 * (p - i) + b

        @pl.when((i <= p) & first_up)
        def _():
            kv_copy(i, j, sem_z, up).wait_send()
            st_copy(i, j, sem_zs, up).wait_send()

        @pl.when((i <= p) & ((i > 0) | (b == 0)))
        def _():
            kv_copy(i, j, sem_y, side).wait_send()
            st_copy(i, j, sem_ys, side).wait_send()


def merge_kernel(ntp, mix_ref, wd_ref, wr_ref, out_ref, wbuf, mine, sent, from_pair, from_chip,
                 wsem, pair_send, pair_recv, chip_send, chip_recv):
    me = lax.axis_index("tp")
    core = lax.rem(me, 2)
    chip = me // 2
    nchip = ntp // 2
    pair = {"tp": me + 1 - 2 * core}
    rows, width = out_ref.shape
    depth = wd_ref.shape[0]
    cut = mine.shape[2]
    pieces = width // cut
    barrier = pltpu.get_barrier_semaphore()
    pl.semaphore_signal(barrier, inc=1, device_id=pair, device_id_type=MESH)
    for d in range(1, nchip):
        there = lax.rem(chip + d, nchip) * 2 + core
        pl.semaphore_signal(barrier, inc=1, device_id={"tp": there}, device_id_type=MESH)
    loads = [
        pltpu.make_async_copy(wd_ref, wbuf.at[:depth], wsem.at[0]),
        pltpu.make_async_copy(wr_ref, wbuf.at[depth:], wsem.at[1]),
    ]
    for load in loads:
        load.start()
    for load in loads:
        load.wait()
    pl.semaphore_wait(barrier, nchip)

    def partial(owner, n):
        part = mix_ref[pl.ds(pl.multiple_of(owner * rows, rows), rows), :]
        return nn(part, wbuf[:, n * cut : (n + 1) * cut])

    def pair_copy(d, n):
        return remote(mine.at[d * pieces + n], from_pair.at[d * pieces + n], pair_send.at[d, n],
                      pair_recv.at[d, n], pair)

    def chip_copy(d, n):
        there = lax.rem(chip + d, nchip) * 2 + core
        return remote(sent.at[d * pieces + n], from_chip.at[d * pieces + n], chip_send.at[d, n],
                      chip_recv.at[d, n], {"tp": there})

    order = list(range(1, nchip)) + [0]
    for d in order:
        target = lax.rem(chip + d, nchip) * 2
        for n in range(pieces):
            mine[d * pieces + n] = partial(target + 1 - core, n).astype(BF16)
            pair_copy(d, n).start()
        if d:
            for n in range(pieces):
                ours = partial(target + core, n)
                pair_copy(d, n).wait_recv()
                sent[d * pieces + n] = (ours + from_pair[d * pieces + n].astype(F32)).astype(BF16)
                chip_copy(d, n).start()
    for n in range(pieces):
        total = partial(me, n)
        pair_copy(0, n).wait_recv()
        total = total + from_pair[n].astype(F32)
        for d in range(1, nchip):
            chip_copy(d, n).wait_recv()
            total = total + from_chip[d * pieces + n].astype(F32)
        out_ref[:, n * cut : (n + 1) * cut] = total.astype(BF16)
    for d in order:
        for n in range(pieces):
            pair_copy(d, n).wait_send()
            if d:
                chip_copy(d, n).wait_send()


VMEM = pl.BlockSpec(memory_space=pltpu.VMEM)
ANY = pl.BlockSpec(memory_space=pl.ANY)
SMEM = pl.BlockSpec(memory_space=pltpu.SMEM)
DMA = pltpu.SemaphoreType.DMA


def params(number):
    return pltpu.CompilerParams(
        collective_id=number, has_side_effects=True, vmem_limit_bytes=VMEM_LIMIT
    )


def on_device(nsp, ntp, tokens, norm_gain, w_query_one, w_query_two, w_key_one, w_key_two, w_value,
              mix_lambda, head_gain, w_ret_query, w_ret_key, w_ret_value, retain_log, init_state,
              w_out_diff, w_out_ret):
    weights = (w_query_one, w_query_two, w_key_one, w_key_two, w_value, w_ret_query, w_ret_key, w_ret_value)
    widths = tuple(w.shape[1] for w in weights)
    own_rows, model = tokens.shape
    rows = own_rows * ntp
    nchip = ntp // 2
    q, kv, r = pl.pallas_call(
        functools.partial(project_kernel, ntp, widths),
        out_shape=[
            jax.ShapeDtypeStruct((rows, sum(widths[:2])), BF16),
            jax.ShapeDtypeStruct((rows, sum(widths[2:5])), BF16),
            jax.ShapeDtypeStruct((rows, sum(widths[5:])), BF16),
        ],
        in_specs=[VMEM, VMEM] + [ANY] * len(weights),
        out_specs=[VMEM] * 3,
        scratch_shapes=[
            pltpu.VMEM((ntp, own_rows, model), BF16),
            pltpu.VMEM((model, sum(widths)), BF16),
            DMA((len(weights),)),
            DMA((nchip, 2)),
            DMA((nchip, 2)),
            DMA((ntp, 2)),
        ],
        compiler_params=params(0),
        name="project",
    )(tokens, norm_gain[None, :], *weights)
    heads = mix_lambda.shape[0]
    rheads, hd, val = init_state.shape
    kw = widths[2]
    npair = nsp // 2
    mixers = pl.pallas_call(
        functools.partial(mix_kernel, nsp, heads, rheads),
        out_shape=jax.ShapeDtypeStruct((rows, (heads + rheads) * val), BF16),
        in_specs=[SMEM, VMEM, VMEM, VMEM, VMEM, VMEM, ANY],
        out_specs=VMEM,
        scratch_shapes=[
            pltpu.VMEM((nsp, rows, kv.shape[1]), BF16),
            pltpu.VMEM((nsp, rheads * hd + 32 * rheads, val), BF16),
            pltpu.VMEM((2 * heads, rows, kw), BF16),
            pltpu.VMEM((2 * heads, rows, 128), F32),
            pltpu.VMEM((2 * heads, rows, 128), F32),
            pltpu.VMEM((2 * heads, rows, val), F32),
            pltpu.VMEM((rheads, rows, val), F32),
            pltpu.VMEM((rheads, rows // BLOCK, rheads * hd, val), F32),
            DMA,
            DMA((npair + 1,)),
            DMA((npair + 1,)),
            DMA((nsp,)),
            DMA((npair + 1,)),
            DMA((npair + 1,)),
            DMA((nsp,)),
        ],
        compiler_params=params(1),
        name="mixers",
    )(mix_lambda, head_gain[None, :], retain_log, init_state, q, r, kv)
    width = w_out_diff.shape[1]
    pieces = 4
    cut = width // pieces
    return pl.pallas_call(
        functools.partial(merge_kernel, ntp),
        out_shape=jax.ShapeDtypeStruct((own_rows, width), BF16),
        in_specs=[VMEM, ANY, ANY],
        out_specs=VMEM,
        scratch_shapes=[
            pltpu.VMEM((w_out_diff.shape[0] + w_out_ret.shape[0], width), BF16),
            pltpu.VMEM((nchip * pieces, own_rows, cut), BF16),
            pltpu.VMEM((nchip * pieces, own_rows, cut), BF16),
            pltpu.VMEM((nchip * pieces, own_rows, cut), BF16),
            pltpu.VMEM((nchip * pieces, own_rows, cut), BF16),
            DMA((2,)),
            DMA((nchip, pieces)),
            DMA((nchip, pieces)),
            DMA((nchip, pieces)),
            DMA((nchip, pieces)),
        ],
        compiler_params=params(2),
        name="merge",
    )(mixers, w_out_diff, w_out_ret)


def solution(mesh):
    in_specs = (
        P(("sp", "tp"), None),
        P(),
        P(None, "tp"),
        P(None, "tp"),
        P(None, "tp"),
        P(None, "tp"),
        P(None, "tp"),
        P("tp"),
        P(),
        P(None, "tp"),
        P(None, "tp"),
        P(None, "tp"),
        P("tp", "sp"),
        P("tp", None, None),
        P("tp", None),
        P("tp", None),
    )
    body = functools.partial(on_device, mesh.shape["sp"], mesh.shape["tp"])
    return jax.shard_map(
        body, mesh=mesh, in_specs=in_specs, out_specs=P(("sp", "tp"), None), check_vma=False
    )
```

```python
import functools

import jax
import jax.numpy as jnp
from jax import lax
from jax.experimental import pallas as pl
from jax.experimental.pallas import tpu as pltpu
from jax.sharding import PartitionSpec as P

BLOCK = 256
NORM_EPS = 1e-06
HEAD_EPS = 1e-05
DIFF_SCALE = 0.8
HIGHEST = lax.Precision.HIGHEST
MESH = pl.DeviceIdType.MESH
F32 = jnp.float32
BF16 = jnp.bfloat16
VMEM_LIMIT = 60 * 1024 * 1024


def remote(src, dst, send, recv, where):
    return pltpu.make_async_remote_copy(
        src_ref=src, dst_ref=dst, send_sem=send, recv_sem=recv,
        device_id=where, device_id_type=MESH,
    )


def head_norm(values):
    return values * lax.rsqrt(jnp.mean(values * values, axis=-1, keepdims=True) + HEAD_EPS)


def nn(a, b, **kw):
    return lax.dot_general(a, b, (((1,), (0,)), ((), ())), preferred_element_type=F32, **kw)


def nt(a, b):
    return lax.dot_general(a, b, (((1,), (1,)), ((), ())), preferred_element_type=F32)


def tn(a, b):
    return lax.dot_general(a, b, (((0,), (0,)), ((), ())), preferred_element_type=F32)


def layer_kernel(nsp, ntp, widths, heads, rheads, lam_ref, tokens_ref, ngain_ref, gain_ref, log_ref,
                 init_ref, *refs):
    nw = len(widths)
    w_refs = refs[:nw]
    wd_ref, wr_ref, out_ref = refs[nw : nw + 3]
    (gat, wbuf, wobuf, kvs, sts, rbuf, qs, peak, den, acc, rmid, upd, mix, mine, sent, from_pair,
     from_chip, wsem, pair_send, cross_send, grecv, sem_z, sem_y, sem_rk, sem_zs, sem_ys, sem_rs,
     mpair_send, mpair_recv, mchip_send, mchip_recv) = refs[nw + 3 :]
    me = lax.axis_index("sp")
    b = lax.rem(me, 2)
    p = me // 2
    npair = nsp // 2
    up = {"sp": lax.rem(me + 2, nsp)}
    side = {"sp": me + 1 - 2 * b}
    tme = lax.axis_index("tp")
    core = lax.rem(tme, 2)
    chip = tme // 2
    nchip = ntp // 2
    tpair = tme + 1 - 2 * core
    pair = {"tp": tpair}
    own_rows = tokens_ref.shape[0]
    rows = own_rows * ntp
    chunk = rows // nchip
    kw = widths[2]
    hd = kw // heads
    val = gain_ref.shape[1]
    first_up = p < npair - 1

    barrier = pltpu.get_barrier_semaphore()

    def greet(where):
        pl.semaphore_signal(barrier, inc=1, device_id=where, device_id_type=MESH)

    greet(side)

    @pl.when(p > 0)
    def _():
        greet({"sp": lax.rem(me + nsp - 2, nsp)})

    @pl.when(first_up)
    def _():
        greet(up)

    greet(pair)
    for d in range(1, nchip):
        greet({"tp": lax.rem(chip + d, nchip) * 2 + core})

    order = (2, 3, 4, 0, 1, 5, 6, 7)
    starts = [sum(widths[:n]) for n in range(nw)]
    loads = {}
    for n in order:
        at = starts[n]
        loads[n] = pltpu.make_async_copy(w_refs[n], wbuf.at[:, at : at + widths[n]], wsem.at[n])
        loads[n].start()
    depth = wd_ref.shape[0]
    out_loads = [
        pltpu.make_async_copy(wd_ref, wobuf.at[:depth], wsem.at[nw]),
        pltpu.make_async_copy(wr_ref, wobuf.at[depth:], wsem.at[nw + 1]),
    ]
    for load in out_loads:
        load.start()
    floats = tokens_ref[...].astype(F32)
    gat[tme] = (
        floats * lax.rsqrt(jnp.mean(floats * floats, axis=-1, keepdims=True) + NORM_EPS) * ngain_ref[...]
    ).astype(BF16)
    pl.semaphore_wait(
        barrier, 1 + nchip + jnp.minimum(p, 1) + jnp.minimum(npair - 1 - p, 1)
    )
    copies = []

    def slab(which, half):
        return gat.at[which, pl.ds(half * (own_rows // 2), own_rows // 2)]

    for d in range(1, nchip):
        there = {"tp": lax.rem(chip + d, nchip) * 2 + core}
        for half in range(2):
            copies.append(remote(slab(tme, half), slab(tme, half), cross_send.at[d, half],
                                 grecv.at[tme, half], there))
            copies[-1].start()

    def to_pair(which, half):
        copies.append(remote(slab(which, half), slab(which, half), pair_send.at[which // 2, half],
                             grecv.at[which, half], pair))
        copies[-1].start()

    def landed(which, half):
        remote(slab(which, half), slab(which, half), pair_send.at[which // 2, half],
               grecv.at[which, half], pair).wait_recv()

    def keys_at(d):
        which = lax.rem(chip + nchip - d, nchip)
        return pl.ds(pl.multiple_of(which * chunk, chunk), chunk)

    def kv_copy(i, j, d, sem, where):
        piece = kvs.at[j, keys_at(d)]
        return remote(piece, piece, sem.at[i, d], sem_rk.at[j, d], where)

    def st_copy(i, j, sem, where):
        return remote(sts.at[j], sts.at[j], sem.at[i], sem_rs.at[j], where)

    qlane = lax.broadcasted_iota(jnp.int32, (chunk, kw), 1)

    def project(d):
        which = lax.rem(chip + nchip - d, nchip)
        both = gat[pl.ds(which * 2, 2)].reshape(chunk, gat.shape[2])
        at = keys_at(d)

        def run(lo, hi, put):
            if d == 0:
                for n in range(lo, hi):
                    loads[n].wait()
            span = sum(widths[lo:hi])
            cut = 256 if span % 256 == 0 else span
            for c in range(0, span, cut):
                put(c, cut, nn(both, wbuf[:, starts[lo] + c : starts[lo] + c + cut]).astype(BF16))

        def put_kv(c, cut, value):
            kvs[me, at, c : c + cut] = value

        def put_r(c, cut, value):
            rbuf[at, c : c + cut] = value

        run(2, 5, put_kv)
        for m in range(2):
            if d == 0:
                loads[m].wait()
            piece = nn(both, wbuf[:, starts[m] : starts[m] + kw]).astype(BF16).astype(F32) * hd ** (-0.5)
            for h in range(heads):
                keep = (qlane >= h * hd) & (qlane < (h + 1) * hd)
                qs[m * heads + h, at, :] = jnp.where(keep, piece, 0.0).astype(BF16)

        @pl.when(first_up)
        def _():
            kv_copy(0, me, d, sem_z, up).start()

        @pl.when(b == 0)
        def _():
            kv_copy(0, me, d, sem_y, side).start()

        run(5, 8, put_r)

    def forward(i, d):
        jz = 2 * (p - i) + b

        @pl.when(i <= p)
        def _():
            kv_copy(i, jz, d, sem_z, up).wait_recv()

            @pl.when(first_up)
            def _():
                kv_copy(i, jz, d, sem_z, up).start()

            kv_copy(i, jz, d, sem_y, side).start()

    for half in range(2):
        to_pair(tme, half)
    for half in range(2):
        landed(tpair, half)
    project(0)
    peak[...] = jnp.full(peak.shape, -jnp.inf, F32)
    den[...] = jnp.zeros(den.shape, F32)
    acc[...] = jnp.zeros(acc.shape, F32)
    forward(1, 0)
    for d in range(1, nchip):
        other = lax.rem(chip + nchip - d, nchip)
        for half in range(2):
            landed(other * 2 + core, half)
            to_pair(other * 2 + core, half)
        for half in range(2):
            landed(other * 2 + 1 - core, half)
        project(d)
    ahead = min(2, npair)
    for i in range(2, ahead + 1):
        forward(i, 0)

    blk = BLOCK
    nblk = rows // blk
    rkw = rheads * hd
    tt = lax.broadcasted_iota(jnp.int32, (blk, blk), 0)
    uu = lax.broadcasted_iota(jnp.int32, (blk, blk), 1)
    lane = lax.broadcasted_iota(jnp.int32, (blk, rkw), 1)
    srow = lax.broadcasted_iota(jnp.int32, (rkw, val), 0)
    decays = []
    span_state = jnp.zeros((rkw, val), F32)
    span_logs = []
    for h in range(rheads):
        ours = (lane >= h * hd) & (lane < (h + 1) * hd)
        keep = (srow >= h * hd) & (srow < (h + 1) * hd)
        state = jnp.zeros((rkw, val), F32)
        log_all = jnp.zeros((1, 1), F32)
        for n in range(nblk):
            at = slice(n * blk, (n + 1) * blk)
            row = log_ref[h : h + 1, at]
            full = jnp.broadcast_to(row, (blk, blk))
            c_col = jnp.sum(jnp.where(uu <= tt, full, 0.0), axis=1, keepdims=True)
            l_col = jnp.sum(jnp.where(uu == tt, full, 0.0), axis=1, keepdims=True)
            c_row = jnp.sum(jnp.where(tt <= uu, l_col, 0.0), axis=0, keepdims=True)
            last = c_col[blk - 1 : blk, :]
            query = jnp.where(ours, rbuf[at, :rkw].astype(F32), 0.0)
            keys = rbuf[at, rkw : 2 * rkw]
            values = rbuf[at, 2 * rkw + h * val : 2 * rkw + (h + 1) * val]
            raw = nt(query.astype(BF16), keys)
            gap = jnp.where(uu <= tt, c_col - c_row, -jnp.inf)
            g = (raw * hd ** (-0.5) * jnp.exp(gap)).astype(BF16)
            rmid[h, at, :] = nn(g, values)
            kd = (keys.astype(F32) * hd ** (-0.5) * jnp.exp(last - c_col)).astype(BF16)
            new = jnp.where(keep, tn(kd, values), 0.0)
            upd[h, n] = new
            state = jnp.exp(last) * state + new
            log_all = log_all + last
            decays.append((c_col, last))
        span_state = span_state + state
        span_logs.append(log_all)
    sts[me, :rkw, :] = span_state.astype(BF16)
    for h in range(rheads):
        wide = jnp.broadcast_to(span_logs[h], (16, val))
        hi = wide.astype(BF16)
        sts[me, rkw + 32 * h : rkw + 32 * h + 16, :] = hi
        sts[me, rkw + 32 * h + 16 : rkw + 32 * h + 32, :] = (wide - hi.astype(F32)).astype(BF16)

    qb = min(rows, 256)

    def attend(j, d):
        diagonal = d is None

        @pl.loop(0, 2 * heads)
        def _(mh):
            m = mh // heads
            h = lax.rem(mh, heads)
            kcol = pl.ds(pl.multiple_of(m * kw, kw), kw)
            vcol = pl.ds(pl.multiple_of(2 * kw + h * val, val), val)
            for n in range(rows // qb):
                at = slice(n * qb, (n + 1) * qb)
                count = (n + 1) * qb if diagonal else chunk
                krows = slice(0, count) if diagonal else keys_at(d)
                scores = nt(qs[mh, at, :], kvs[j, krows, kcol])
                if diagonal:
                    ti = lax.broadcasted_iota(jnp.int32, (qb, count), 0) + n * qb
                    ui = lax.broadcasted_iota(jnp.int32, (qb, count), 1)
                    scores = jnp.where(ui <= ti, scores, -jnp.inf)
                old = peak[mh, at, :]
                top = jnp.maximum(old, jnp.max(scores, axis=1, keepdims=True))
                e = jnp.exp(scores - top[:, :1])
                part = e[:, :128]
                for c in range(128, count, 128):
                    part = part + e[:, c : c + 128]
                weighted = nn(e.astype(BF16), kvs[j, krows, vcol])
                rescale = jnp.exp(old - top)
                peak[mh, at, :] = top
                den[mh, at, :] = den[mh, at, :] * rescale + part
                acc[mh, at, :] = acc[mh, at, :] * rescale[:, :1] + weighted

    attend(me, None)

    @pl.when(first_up)
    def _():
        st_copy(0, me, sem_zs, up).start()

    @pl.when(b == 0)
    def _():
        st_copy(0, me, sem_ys, side).start()

    for d in range(nchip):
        @pl.loop(1, npair + 1)
        def _(i):
            jz = 2 * (p - i) + b
            jy = 2 * (p - i + 1) + 1 - b
            if d == 0:
                @pl.when(i > ahead)
                def _():
                    forward(i, 0)
            else:
                forward(i, d)

            @pl.when(i <= p)
            def _():
                if d == nchip - 1:
                    st_copy(i, jz, sem_zs, up).wait_recv()

                    @pl.when(first_up)
                    def _():
                        st_copy(i, jz, sem_zs, up).start()

                    st_copy(i, jz, sem_ys, side).start()
                attend(jz, d)

            @pl.when((i - 1 <= p) & ((b == 1) | (i > 1)))
            def _():
                kv_copy(i, jy, d, sem_y, side).wait_recv()
                if d == nchip - 1:
                    st_copy(i, jy, sem_ys, side).wait_recv()
                attend(jy, d)

    first = []
    for h in range(rheads):
        parts = [jnp.zeros((hd, val), F32)] * h + [init_ref[h]] + [jnp.zeros((hd, val), F32)] * (rheads - 1 - h)
        first.append(jnp.concatenate(parts, axis=0) if rheads > 1 else parts[0])

    def join(j, states):
        out = []
        for h in range(rheads):
            keep = (srow >= h * hd) & (srow < (h + 1) * hd)
            base = rkw + 32 * h
            log = sts[j, base : base + 16, :].astype(F32) + sts[j, base + 16 : base + 32, :].astype(F32)
            piece = jnp.where(keep, sts[j, :rkw, :].astype(F32), 0.0)
            out.append(jnp.exp(log[:1, :]) * states[h] + piece)
        return tuple(out)

    carried = lax.fori_loop(0, me, join, tuple(first))
    for h in range(rheads):
        state = carried[h]
        for n in range(nblk):
            at = slice(n * blk, (n + 1) * blk)
            c_col, last = decays[h * nblk + n]
            query = rbuf[at, :rkw].astype(F32) * jnp.exp(c_col)
            result = rmid[h, at, :] + nn(query, state, precision=HIGHEST)
            if n + 1 < nblk:
                state = jnp.exp(last) * state + upd[h, n]
            mix[at, heads * val + h * val : heads * val + (h + 1) * val] = head_norm(result).astype(BF16)
    for h in range(heads):
        pieces = []
        for m in range(2):
            mh = m * heads + h
            total = jnp.sum(den[mh], axis=1, keepdims=True)
            pieces.append(acc[mh] / total)
        mixed = pieces[0] - lam_ref[h] * pieces[1]
        mix[:, h * val : (h + 1) * val] = (head_norm(mixed) * gain_ref[...] * DIFF_SCALE).astype(BF16)
    for load in out_loads:
        load.wait()

    width = out_ref.shape[1]
    cut = mine.shape[2]
    npiece = width // cut

    def partial(owner, n):
        part = mix[pl.ds(pl.multiple_of(owner * own_rows, own_rows), own_rows), :]
        return nn(part, wobuf[:, n * cut : (n + 1) * cut])

    def pair_copy(d, n):
        return remote(mine.at[d * npiece + n], from_pair.at[d * npiece + n], mpair_send.at[d, n],
                      mpair_recv.at[d, n], pair)

    def chip_copy(d, n):
        there = lax.rem(chip + d, nchip) * 2 + core
        return remote(sent.at[d * npiece + n], from_chip.at[d * npiece + n], mchip_send.at[d, n],
                      mchip_recv.at[d, n], {"tp": there})

    targets = list(range(1, nchip)) + [0]
    for d in targets:
        target = lax.rem(chip + d, nchip) * 2
        for n in range(npiece):
            mine[d * npiece + n] = partial(target + 1 - core, n).astype(BF16)
            pair_copy(d, n).start()
        if d:
            for n in range(npiece):
                ours = partial(target + core, n)
                pair_copy(d, n).wait_recv()
                sent[d * npiece + n] = (ours + from_pair[d * npiece + n].astype(F32)).astype(BF16)
                chip_copy(d, n).start()
    for n in range(npiece):
        total = partial(tme, n)
        pair_copy(0, n).wait_recv()
        total = total + from_pair[n].astype(F32)
        for d in range(1, nchip):
            chip_copy(d, n).wait_recv()
            total = total + from_chip[d * npiece + n].astype(F32)
        out_ref[:, n * cut : (n + 1) * cut] = total.astype(BF16)

    for copy in copies:
        copy.wait_send()

    @pl.loop(0, npair)
    def _(i):
        j = 2 * (p - i) + b

        @pl.when((i <= p) & first_up)
        def _():
            for d in range(nchip):
                kv_copy(i, j, d, sem_z, up).wait_send()
            st_copy(i, j, sem_zs, up).wait_send()

        @pl.when((i <= p) & ((i > 0) | (b == 0)))
        def _():
            for d in range(nchip):
                kv_copy(i, j, d, sem_y, side).wait_send()
            st_copy(i, j, sem_ys, side).wait_send()

    for d in targets:
        for n in range(npiece):
            pair_copy(d, n).wait_send()
            if d:
                chip_copy(d, n).wait_send()


VMEM = pl.BlockSpec(memory_space=pltpu.VMEM)
ANY = pl.BlockSpec(memory_space=pl.ANY)
SMEM = pl.BlockSpec(memory_space=pltpu.SMEM)
DMA = pltpu.SemaphoreType.DMA


def params(number):
    return pltpu.CompilerParams(
        collective_id=number, has_side_effects=True, vmem_limit_bytes=VMEM_LIMIT
    )


def on_device(nsp, ntp, tokens, norm_gain, w_query_one, w_query_two, w_key_one, w_key_two, w_value,
              mix_lambda, head_gain, w_ret_query, w_ret_key, w_ret_value, retain_log, init_state,
              w_out_diff, w_out_ret):
    weights = (w_query_one, w_query_two, w_key_one, w_key_two, w_value, w_ret_query, w_ret_key, w_ret_value)
    widths = tuple(w.shape[1] for w in weights)
    own_rows, model = tokens.shape
    rows = own_rows * ntp
    nchip = ntp // 2
    npair = nsp // 2
    heads = mix_lambda.shape[0]
    rheads, hd, val = init_state.shape
    kw = widths[2]
    width = w_out_diff.shape[1]
    npiece = 4
    cut = width // npiece
    return pl.pallas_call(
        functools.partial(layer_kernel, nsp, ntp, widths, heads, rheads),
        out_shape=jax.ShapeDtypeStruct((own_rows, width), BF16),
        in_specs=[SMEM] + [VMEM] * 5 + [ANY] * (len(weights) + 2),
        out_specs=VMEM,
        scratch_shapes=[
            pltpu.VMEM((ntp, own_rows, model), BF16),
            pltpu.VMEM((model, sum(widths)), BF16),
            pltpu.VMEM((w_out_diff.shape[0] + w_out_ret.shape[0], width), BF16),
            pltpu.VMEM((nsp, rows, sum(widths[2:5])), BF16),
            pltpu.VMEM((nsp, rheads * hd + 32 * rheads, val), BF16),
            pltpu.VMEM((rows, sum(widths[5:])), BF16),
            pltpu.VMEM((2 * heads, rows, kw), BF16),
            pltpu.VMEM((2 * heads, rows, 128), F32),
            pltpu.VMEM((2 * heads, rows, 128), F32),
            pltpu.VMEM((2 * heads, rows, val), F32),
            pltpu.VMEM((rheads, rows, val), F32),
            pltpu.VMEM((rheads, rows // BLOCK, rheads * hd, val), F32),
            pltpu.VMEM((rows, (heads + rheads) * val), BF16),
            pltpu.VMEM((nchip * npiece, own_rows, cut), BF16),
            pltpu.VMEM((nchip * npiece, own_rows, cut), BF16),
            pltpu.VMEM((nchip * npiece, own_rows, cut), BF16),
            pltpu.VMEM((nchip * npiece, own_rows, cut), BF16),
            DMA((len(weights) + 2,)),
            DMA((nchip, 2)),
            DMA((nchip, 2)),
            DMA((ntp, 2)),
            DMA((npair + 1, nchip)),
            DMA((npair + 1, nchip)),
            DMA((nsp, nchip)),
            DMA((npair + 1,)),
            DMA((npair + 1,)),
            DMA((nsp,)),
            DMA((nchip, npiece)),
            DMA((nchip, npiece)),
            DMA((nchip, npiece)),
            DMA((nchip, npiece)),
        ],
        compiler_params=params(0),
        name="layer",
    )(mix_lambda, tokens, norm_gain[None, :], head_gain[None, :], retain_log, init_state, *weights,
      w_out_diff, w_out_ret)


def solution(mesh):
    in_specs = (
        P(("sp", "tp"), None),
        P(),
        P(None, "tp"),
        P(None, "tp"),
        P(None, "tp"),
        P(None, "tp"),
        P(None, "tp"),
        P("tp"),
        P(),
        P(None, "tp"),
        P(None, "tp"),
        P(None, "tp"),
        P("tp", "sp"),
        P("tp", None, None),
        P("tp", None),
        P("tp", None),
    )
    body = functools.partial(on_device, mesh.shape["sp"], mesh.shape["tp"])
    return jax.shard_map(
        body, mesh=mesh, in_specs=in_specs, out_specs=P(("sp", "tp"), None), check_vma=False
    )
```

```python
import functools

import jax
import jax.numpy as jnp
from jax import lax
from jax.experimental import pallas as pl
from jax.experimental.pallas import tpu as pltpu
from jax.sharding import PartitionSpec as P

BLOCK = 256
NORM_EPS = 1e-06
HEAD_EPS = 1e-05
DIFF_SCALE = 0.8
HIGHEST = lax.Precision.HIGHEST
MESH = pl.DeviceIdType.MESH
F32 = jnp.float32
BF16 = jnp.bfloat16
VMEM_LIMIT = 60 * 1024 * 1024


def remote(src, dst, send, recv, where):
    return pltpu.make_async_remote_copy(
        src_ref=src, dst_ref=dst, send_sem=send, recv_sem=recv,
        device_id=where, device_id_type=MESH,
    )


def head_norm(values):
    return values * lax.rsqrt(jnp.mean(values * values, axis=-1, keepdims=True) + HEAD_EPS)


def nn(a, b, **kw):
    return lax.dot_general(a, b, (((1,), (0,)), ((), ())), preferred_element_type=F32, **kw)


def nt(a, b):
    return lax.dot_general(a, b, (((1,), (1,)), ((), ())), preferred_element_type=F32)


def tn(a, b):
    return lax.dot_general(a, b, (((0,), (0,)), ((), ())), preferred_element_type=F32)


def layer_kernel(nsp, ntp, widths, heads, rheads, lam_ref, tokens_ref, ngain_ref, gain_ref, log_ref,
                 init_ref, *refs):
    nw = len(widths)
    w_refs = refs[:nw]
    wd_ref, wr_ref, out_ref = refs[nw : nw + 3]
    (gat, wbuf, wobuf, kvs, sts, rbuf, qs, peak, den, acc, rmid, upd, mix, mine, sent, from_pair,
     from_chip, wsem, pair_send, cross_send, grecv, sem_z, sem_y, sem_rk, sem_zs, sem_ys, sem_rs,
     mpair_send, mpair_recv, mchip_send, mchip_recv) = refs[nw + 3 :]
    me = lax.axis_index("sp")
    b = lax.rem(me, 2)
    p = me // 2
    npair = nsp // 2
    up = {"sp": lax.rem(me + 2, nsp)}
    side = {"sp": me + 1 - 2 * b}
    tme = lax.axis_index("tp")
    core = lax.rem(tme, 2)
    chip = tme // 2
    nchip = ntp // 2
    tpair = tme + 1 - 2 * core
    pair = {"tp": tpair}
    own_rows = tokens_ref.shape[0]
    rows = own_rows * ntp
    chunk = rows // nchip
    kw = widths[2]
    hd = kw // heads
    val = gain_ref.shape[1]
    first_up = p < npair - 1

    barrier = pltpu.get_barrier_semaphore()

    def greet(where):
        pl.semaphore_signal(barrier, inc=1, device_id=where, device_id_type=MESH)

    greet(side)

    @pl.when(p > 0)
    def _():
        greet({"sp": lax.rem(me + nsp - 2, nsp)})

    @pl.when(first_up)
    def _():
        greet(up)

    greet(pair)
    for d in range(1, nchip):
        greet({"tp": lax.rem(chip + d, nchip) * 2 + core})

    order = (2, 3, 4, 0, 1, 5, 6, 7)
    starts = [sum(widths[:n]) for n in range(nw)]
    loads = {}
    for n in order:
        at = starts[n]
        loads[n] = pltpu.make_async_copy(w_refs[n], wbuf.at[:, at : at + widths[n]], wsem.at[n])
        loads[n].start()
    depth = wd_ref.shape[0]
    out_loads = [
        pltpu.make_async_copy(wd_ref, wobuf.at[:depth], wsem.at[nw]),
        pltpu.make_async_copy(wr_ref, wobuf.at[depth:], wsem.at[nw + 1]),
    ]
    for load in out_loads:
        load.start()
    floats = tokens_ref[...].astype(F32)
    gat[tme] = (
        floats * lax.rsqrt(jnp.mean(floats * floats, axis=-1, keepdims=True) + NORM_EPS) * ngain_ref[...]
    ).astype(BF16)
    pl.semaphore_wait(
        barrier, 1 + nchip + jnp.minimum(p, 1) + jnp.minimum(npair - 1 - p, 1)
    )
    copies = []

    def slab(which, half):
        return gat.at[which, pl.ds(half * (own_rows // 2), own_rows // 2)]

    for d in range(1, nchip):
        there = {"tp": lax.rem(chip + d, nchip) * 2 + core}
        for half in range(2):
            copies.append(remote(slab(tme, half), slab(tme, half), cross_send.at[d, half],
                                 grecv.at[tme, half], there))
            copies[-1].start()

    def to_pair(which, half):
        copies.append(remote(slab(which, half), slab(which, half), pair_send.at[which // 2, half],
                             grecv.at[which, half], pair))
        copies[-1].start()

    def landed(which, half):
        remote(slab(which, half), slab(which, half), pair_send.at[which // 2, half],
               grecv.at[which, half], pair).wait_recv()

    def keys_at(d):
        which = lax.rem(chip + nchip - d, nchip)
        return pl.ds(pl.multiple_of(which * chunk, chunk), chunk)

    def kv_copy(i, j, d, sem, where):
        piece = kvs.at[j, keys_at(d)]
        return remote(piece, piece, sem.at[i, d], sem_rk.at[j, d], where)

    def st_copy(i, j, sem, where):
        return remote(sts.at[j], sts.at[j], sem.at[i], sem_rs.at[j], where)

    qlane = lax.broadcasted_iota(jnp.int32, (chunk, kw), 1)

    def project(d):
        which = lax.rem(chip + nchip - d, nchip)
        both = gat[pl.ds(which * 2, 2)].reshape(chunk, gat.shape[2])
        at = keys_at(d)

        def run(lo, hi, put):
            if d == 0:
                for n in range(lo, hi):
                    loads[n].wait()
            span = sum(widths[lo:hi])
            cut = 256 if span % 256 == 0 else span
            for c in range(0, span, cut):
                put(c, cut, nn(both, wbuf[:, starts[lo] + c : starts[lo] + c + cut]).astype(BF16))

        def put_kv(c, cut, value):
            kvs[me, at, c : c + cut] = value

        def put_r(c, cut, value):
            rbuf[at, c : c + cut] = value

        run(2, 5, put_kv)
        for m in range(2):
            if d == 0:
                loads[m].wait()
            piece = nn(both, wbuf[:, starts[m] : starts[m] + kw]).astype(BF16).astype(F32) * hd ** (-0.5)
            for h in range(heads):
                keep = (qlane >= h * hd) & (qlane < (h + 1) * hd)
                qs[m * heads + h, at, :] = jnp.where(keep, piece, 0.0).astype(BF16)

        @pl.when(first_up)
        def _():
            kv_copy(0, me, d, sem_z, up).start()

        @pl.when(b == 0)
        def _():
            kv_copy(0, me, d, sem_y, side).start()

        run(5, 8, put_r)

    def forward(i, d):
        jz = 2 * (p - i) + b

        @pl.when(i <= p)
        def _():
            kv_copy(i, jz, d, sem_z, up).wait_recv()

            @pl.when(first_up)
            def _():
                kv_copy(i, jz, d, sem_z, up).start()

            kv_copy(i, jz, d, sem_y, side).start()

    for half in range(2):
        to_pair(tme, half)
    for half in range(2):
        landed(tpair, half)
    project(0)
    peak[...] = jnp.full(peak.shape, -jnp.inf, F32)
    den[...] = jnp.zeros(den.shape, F32)
    acc[...] = jnp.zeros(acc.shape, F32)
    forward(1, 0)
    for d in range(1, nchip):
        other = lax.rem(chip + nchip - d, nchip)
        for half in range(2):
            landed(other * 2 + core, half)
            to_pair(other * 2 + core, half)
        for half in range(2):
            landed(other * 2 + 1 - core, half)
        project(d)
    if npair > 1:
        forward(2, 0)

    blk = BLOCK
    nblk = rows // blk
    rkw = rheads * hd
    tt = lax.broadcasted_iota(jnp.int32, (blk, blk), 0)
    uu = lax.broadcasted_iota(jnp.int32, (blk, blk), 1)
    lane = lax.broadcasted_iota(jnp.int32, (blk, rkw), 1)
    srow = lax.broadcasted_iota(jnp.int32, (rkw, val), 0)
    decays = []
    span_state = jnp.zeros((rkw, val), F32)
    span_logs = []
    for h in range(rheads):
        ours = (lane >= h * hd) & (lane < (h + 1) * hd)
        keep = (srow >= h * hd) & (srow < (h + 1) * hd)
        state = jnp.zeros((rkw, val), F32)
        log_all = jnp.zeros((1, 1), F32)
        for n in range(nblk):
            at = slice(n * blk, (n + 1) * blk)
            row = log_ref[h : h + 1, at]
            full = jnp.broadcast_to(row, (blk, blk))
            c_col = jnp.sum(jnp.where(uu <= tt, full, 0.0), axis=1, keepdims=True)
            l_col = jnp.sum(jnp.where(uu == tt, full, 0.0), axis=1, keepdims=True)
            c_row = jnp.sum(jnp.where(tt <= uu, l_col, 0.0), axis=0, keepdims=True)
            last = c_col[blk - 1 : blk, :]
            query = jnp.where(ours, rbuf[at, :rkw].astype(F32), 0.0)
            keys = rbuf[at, rkw : 2 * rkw]
            values = rbuf[at, 2 * rkw + h * val : 2 * rkw + (h + 1) * val]
            raw = nt(query.astype(BF16), keys)
            gap = jnp.where(uu <= tt, c_col - c_row, -jnp.inf)
            g = (raw * hd ** (-0.5) * jnp.exp(gap)).astype(BF16)
            rmid[h, at, :] = nn(g, values)
            kd = (keys.astype(F32) * hd ** (-0.5) * jnp.exp(last - c_col)).astype(BF16)
            new = jnp.where(keep, tn(kd, values), 0.0)
            upd[h, n] = new
            state = jnp.exp(last) * state + new
            log_all = log_all + last
            decays.append((c_col, last))
        span_state = span_state + state
        span_logs.append(log_all)
    sts[me, :rkw, :] = span_state.astype(BF16)
    for h in range(rheads):
        wide = jnp.broadcast_to(span_logs[h], (16, val))
        hi = wide.astype(BF16)
        sts[me, rkw + 32 * h : rkw + 32 * h + 16, :] = hi
        sts[me, rkw + 32 * h + 16 : rkw + 32 * h + 32, :] = (wide - hi.astype(F32)).astype(BF16)

    qb = min(rows, 256)

    def attend(j, diagonal):

        @pl.loop(0, 2 * heads)
        def _(mh):
            m = mh // heads
            h = lax.rem(mh, heads)
            kcol = pl.ds(pl.multiple_of(m * kw, kw), kw)
            vcol = pl.ds(pl.multiple_of(2 * kw + h * val, val), val)
            for n in range(rows // qb):
                at = slice(n * qb, (n + 1) * qb)
                count = (n + 1) * qb if diagonal else rows
                krows = slice(0, count)
                scores = nt(qs[mh, at, :], kvs[j, krows, kcol])
                if diagonal:
                    ti = lax.broadcasted_iota(jnp.int32, (qb, count), 0) + n * qb
                    ui = lax.broadcasted_iota(jnp.int32, (qb, count), 1)
                    scores = jnp.where(ui <= ti, scores, -jnp.inf)
                old = peak[mh, at, :]
                top = jnp.maximum(old, jnp.max(scores, axis=1, keepdims=True))
                e = jnp.exp(scores - top[:, :1])
                part = e[:, :128]
                for c in range(128, count, 128):
                    part = part + e[:, c : c + 128]
                weighted = nn(e.astype(BF16), kvs[j, krows, vcol])
                rescale = jnp.exp(old - top)
                peak[mh, at, :] = top
                den[mh, at, :] = den[mh, at, :] * rescale + part
                acc[mh, at, :] = acc[mh, at, :] * rescale[:, :1] + weighted

    @pl.loop(3, npair + 1)
    def _(i):
        forward(i, 0)

    attend(me, True)

    @pl.when(first_up)
    def _():
        st_copy(0, me, sem_zs, up).start()

    @pl.when(b == 0)
    def _():
        st_copy(0, me, sem_ys, side).start()

    @pl.loop(1, npair + 1)
    def _(i):
        jz = 2 * (p - i) + b
        jy = 2 * (p - i + 1) + 1 - b
        for d in range(1, nchip):
            forward(i, d)

        @pl.when(i <= p)
        def _():
            st_copy(i, jz, sem_zs, up).wait_recv()

            @pl.when(first_up)
            def _():
                st_copy(i, jz, sem_zs, up).start()

            st_copy(i, jz, sem_ys, side).start()
            attend(jz, False)

        @pl.when((i - 1 <= p) & ((b == 1) | (i > 1)))
        def _():
            for d in range(nchip):
                kv_copy(i, jy, d, sem_y, side).wait_recv()
            st_copy(i, jy, sem_ys, side).wait_recv()
            attend(jy, False)

    first = []
    for h in range(rheads):
        parts = [jnp.zeros((hd, val), F32)] * h + [init_ref[h]] + [jnp.zeros((hd, val), F32)] * (rheads - 1 - h)
        first.append(jnp.concatenate(parts, axis=0) if rheads > 1 else parts[0])

    def join(j, states):
        out = []
        for h in range(rheads):
            keep = (srow >= h * hd) & (srow < (h + 1) * hd)
            base = rkw + 32 * h
            log = sts[j, base : base + 16, :].astype(F32) + sts[j, base + 16 : base + 32, :].astype(F32)
            piece = jnp.where(keep, sts[j, :rkw, :].astype(F32), 0.0)
            out.append(jnp.exp(log[:1, :]) * states[h] + piece)
        return tuple(out)

    carried = lax.fori_loop(0, me, join, tuple(first))
    for h in range(rheads):
        state = carried[h]
        for n in range(nblk):
            at = slice(n * blk, (n + 1) * blk)
            c_col, last = decays[h * nblk + n]
            query = rbuf[at, :rkw].astype(F32) * jnp.exp(c_col)
            result = rmid[h, at, :] + nn(query, state, precision=HIGHEST)
            if n + 1 < nblk:
                state = jnp.exp(last) * state + upd[h, n]
            mix[at, heads * val + h * val : heads * val + (h + 1) * val] = head_norm(result).astype(BF16)
    for h in range(heads):
        pieces = []
        for m in range(2):
            mh = m * heads + h
            total = jnp.sum(den[mh], axis=1, keepdims=True)
            pieces.append(acc[mh] / total)
        mixed = pieces[0] - lam_ref[h] * pieces[1]
        mix[:, h * val : (h + 1) * val] = (head_norm(mixed) * gain_ref[...] * DIFF_SCALE).astype(BF16)
    for load in out_loads:
        load.wait()

    width = out_ref.shape[1]
    cut = mine.shape[2]
    npiece = width // cut

    def partial(owner, n):
        part = mix[pl.ds(pl.multiple_of(owner * own_rows, own_rows), own_rows), :]
        return nn(part, wobuf[:, n * cut : (n + 1) * cut])

    def pair_copy(d, n):
        return remote(mine.at[d * npiece + n], from_pair.at[d * npiece + n], mpair_send.at[d, n],
                      mpair_recv.at[d, n], pair)

    def chip_copy(d, n):
        there = lax.rem(chip + d, nchip) * 2 + core
        return remote(sent.at[d * npiece + n], from_chip.at[d * npiece + n], mchip_send.at[d, n],
                      mchip_recv.at[d, n], {"tp": there})

    targets = list(range(1, nchip)) + [0]
    for d in targets:
        target = lax.rem(chip + d, nchip) * 2
        for n in range(npiece):
            mine[d * npiece + n] = partial(target + 1 - core, n).astype(BF16)
            pair_copy(d, n).start()
        if d:
            for n in range(npiece):
                ours = partial(target + core, n)
                pair_copy(d, n).wait_recv()
                sent[d * npiece + n] = (ours + from_pair[d * npiece + n].astype(F32)).astype(BF16)
                chip_copy(d, n).start()
    for n in range(npiece):
        total = partial(tme, n)
        pair_copy(0, n).wait_recv()
        total = total + from_pair[n].astype(F32)
        for d in range(1, nchip):
            chip_copy(d, n).wait_recv()
            total = total + from_chip[d * npiece + n].astype(F32)
        out_ref[:, n * cut : (n + 1) * cut] = total.astype(BF16)

    for copy in copies:
        copy.wait_send()

    @pl.loop(0, npair)
    def _(i):
        j = 2 * (p - i) + b

        @pl.when((i <= p) & first_up)
        def _():
            for d in range(nchip):
                kv_copy(i, j, d, sem_z, up).wait_send()
            st_copy(i, j, sem_zs, up).wait_send()

        @pl.when((i <= p) & ((i > 0) | (b == 0)))
        def _():
            for d in range(nchip):
                kv_copy(i, j, d, sem_y, side).wait_send()
            st_copy(i, j, sem_ys, side).wait_send()

    for d in targets:
        for n in range(npiece):
            pair_copy(d, n).wait_send()
            if d:
                chip_copy(d, n).wait_send()


VMEM = pl.BlockSpec(memory_space=pltpu.VMEM)
ANY = pl.BlockSpec(memory_space=pl.ANY)
SMEM = pl.BlockSpec(memory_space=pltpu.SMEM)
DMA = pltpu.SemaphoreType.DMA


def params(number):
    return pltpu.CompilerParams(
        collective_id=number, has_side_effects=True, vmem_limit_bytes=VMEM_LIMIT
    )


def on_device(nsp, ntp, tokens, norm_gain, w_query_one, w_query_two, w_key_one, w_key_two, w_value,
              mix_lambda, head_gain, w_ret_query, w_ret_key, w_ret_value, retain_log, init_state,
              w_out_diff, w_out_ret):
    weights = (w_query_one, w_query_two, w_key_one, w_key_two, w_value, w_ret_query, w_ret_key, w_ret_value)
    widths = tuple(w.shape[1] for w in weights)
    own_rows, model = tokens.shape
    rows = own_rows * ntp
    nchip = ntp // 2
    npair = nsp // 2
    heads = mix_lambda.shape[0]
    rheads, hd, val = init_state.shape
    kw = widths[2]
    width = w_out_diff.shape[1]
    npiece = 4
    cut = width // npiece
    return pl.pallas_call(
        functools.partial(layer_kernel, nsp, ntp, widths, heads, rheads),
        out_shape=jax.ShapeDtypeStruct((own_rows, width), BF16),
        in_specs=[SMEM] + [VMEM] * 5 + [ANY] * (len(weights) + 2),
        out_specs=VMEM,
        scratch_shapes=[
            pltpu.VMEM((ntp, own_rows, model), BF16),
            pltpu.VMEM((model, sum(widths)), BF16),
            pltpu.VMEM((w_out_diff.shape[0] + w_out_ret.shape[0], width), BF16),
            pltpu.VMEM((nsp, rows, sum(widths[2:5])), BF16),
            pltpu.VMEM((nsp, rheads * hd + 32 * rheads, val), BF16),
            pltpu.VMEM((rows, sum(widths[5:])), BF16),
            pltpu.VMEM((2 * heads, rows, kw), BF16),
            pltpu.VMEM((2 * heads, rows, 128), F32),
            pltpu.VMEM((2 * heads, rows, 128), F32),
            pltpu.VMEM((2 * heads, rows, val), F32),
            pltpu.VMEM((rheads, rows, val), F32),
            pltpu.VMEM((rheads, rows // BLOCK, rheads * hd, val), F32),
            pltpu.VMEM((rows, (heads + rheads) * val), BF16),
            pltpu.VMEM((nchip * npiece, own_rows, cut), BF16),
            pltpu.VMEM((nchip * npiece, own_rows, cut), BF16),
            pltpu.VMEM((nchip * npiece, own_rows, cut), BF16),
            pltpu.VMEM((nchip * npiece, own_rows, cut), BF16),
            DMA((len(weights) + 2,)),
            DMA((nchip, 2)),
            DMA((nchip, 2)),
            DMA((ntp, 2)),
            DMA((npair + 1, nchip)),
            DMA((npair + 1, nchip)),
            DMA((nsp, nchip)),
            DMA((npair + 1,)),
            DMA((npair + 1,)),
            DMA((nsp,)),
            DMA((nchip, npiece)),
            DMA((nchip, npiece)),
            DMA((nchip, npiece)),
            DMA((nchip, npiece)),
        ],
        compiler_params=params(0),
        name="layer",
    )(mix_lambda, tokens, norm_gain[None, :], head_gain[None, :], retain_log, init_state, *weights,
      w_out_diff, w_out_ret)


def solution(mesh):
    in_specs = (
        P(("sp", "tp"), None),
        P(),
        P(None, "tp"),
        P(None, "tp"),
        P(None, "tp"),
        P(None, "tp"),
        P(None, "tp"),
        P("tp"),
        P(),
        P(None, "tp"),
        P(None, "tp"),
        P(None, "tp"),
        P("tp", "sp"),
        P("tp", None, None),
        P("tp", None),
        P("tp", None),
    )
    body = functools.partial(on_device, mesh.shape["sp"], mesh.shape["tp"])
    return jax.shard_map(
        body, mesh=mesh, in_specs=in_specs, out_specs=P(("sp", "tp"), None), check_vma=False
    )
```
